32 devices in a mesh: fs: 8 (over z, y), tp: 4 (over x, core).
Axes of the slice: x: 2, y: 2, z: 4, core: 2. Of those that a mesh axis runs over, the one named last changes fastest.
Arguments:
- x_late: bfloat16 [6144, 2048], P(('fs', 'tp')), may hold values from -6 to 6
- x_early: bfloat16 [6144, 2048], P(('fs', 'tp')), may hold values from -6 to 6
- w_gate: bfloat16 [2048, 5632], P('fs', 'tp'), may hold values from -0.125 to 0.125
- w_value: bfloat16 [2048, 5632], P('fs', 'tp'), may hold values from -0.125 to 0.125
- conv_taps: float32 [3, 5632], P(None, 'tp'), may hold values from -3 to 3
- grad_hidden: bfloat16 [6144, 5632], P('fs', 'tp'), may hold values from -6 to 6
- sum_gate: float32 [2048, 5632], P('fs', 'tp'), may hold values from -6 to 6
- sum_value: float32 [2048, 5632], P('fs', 'tp'), may hold values from -6 to 6
- sum_taps: float32 [3, 5632], P(None, 'tp'), may hold values from -6 to 6
Outputs:
- hidden_late: bfloat16 [6144, 5632], P('fs', 'tp')
- grad_early: bfloat16 [6144, 2048], P(('fs', 'tp'))
- new_sum_gate: float32 [2048, 5632], P('fs', 'tp')
- new_sum_value: float32 [2048, 5632], P('fs', 'tp')
- new_sum_taps: float32 [3, 5632], P(None, 'tp')
The draws below stay inside these ranges and needn't reach their ends.
All inputs are finite; a program needn't handle non-finite values.
Results may differ from the reference program's by a relative error of at most 0.015.
Values may be sent and summed in bfloat16 or wider, within the bound.
A program may use at most 128 MiB of HBM per device.

```python
import jax
import jax.numpy as jnp
from jax import lax

D = 2048
FF = 5632
KW = 3
SEQ_LEN = 768
TOKENS = 6144
N_TP = 4


def spiked(entries, own_key, source, target, parts, factor):
    def block_of(position):
        return (jnp.arange(entries.shape[position]) // (entries.shape[position] // parts)).reshape((-1,) + (1,) * (entries.ndim - 1 - position))

    first = jax.random.permutation(own_key, parts)[block_of(target)]
    second = (block_of(target) + parts // 2) % parts
    return jnp.where((block_of(source) == first) | (block_of(source) == second), factor * entries, entries)


def levels(rng, dims, split, low, top_value):
    level, own = 1.0, jax.random.fold_in(rng, 6)
    for axis_at, shards_of in split:
        heights = jnp.exp(jax.random.uniform(jax.random.fold_in(own, axis_at), (shards_of,), jnp.float32, low / len(split), top_value / len(split)))
        level = level * jnp.repeat(heights, dims[axis_at] // shards_of).reshape([-1 if axis == axis_at else 1 for axis in range(len(dims))])
    return level


def scatter_about(rng, shape, deviation, reach, pieces=(), held_as=jnp.bfloat16):
    factor_of = levels(rng, shape, pieces, -0.22, 0.18) if pieces else 1.0
    array = jax.random.normal(rng, shape, jnp.float32) * deviation * factor_of
    return jnp.minimum(jnp.maximum(array, -reach), reach).astype(held_as)


def gaussian_with(key, shape, spread, reach, pieces, heavy, kind=jnp.bfloat16):
    entries = spread * jax.random.normal(key, shape, jnp.float32)
    if pieces:
        entries = entries * levels(key, shape, pieces, -0.22, 0.18)
    return jnp.clip(spiked(entries, jax.random.fold_in(key, 3), *heavy), -reach, reach).astype(kind)


def setup_inputs(seed: int = 0) -> dict:
    key_of = jax.random.split(jax.random.key(seed), 10)
    return {
        "x_late": scatter_about(key_of[0], (TOKENS, D), 1.0, 6.0, ((0, 32),)),
        "x_early": scatter_about(key_of[1], (TOKENS, D), 1.0, 6.0, ((0, 32),)),
        "w_gate": scatter_about(key_of[2], (D, FF), D ** -0.5, 0.125, ((0, 8), (1, 4))),
        "w_value": scatter_about(key_of[3], (D, FF), D ** -0.5, 0.125, ((0, 8), (1, 4))),
        "conv_taps": scatter_about(key_of[4], (KW, FF), 0.6, 3.0, ((1, 4),), jnp.float32),
        "grad_hidden": gaussian_with(key_of[5], (TOKENS, FF), 1.0, 6.0, ((0, 8), (1, 4)), (0, 1, 8, 2.0)),
        "sum_gate": scatter_about(key_of[6], (D, FF), 1.0, 6.0, ((0, 8), (1, 4)), jnp.float32),
        "sum_value": scatter_about(key_of[7], (D, FF), 1.0, 6.0, ((0, 8), (1, 4)), jnp.float32),
        "sum_taps": scatter_about(key_of[8], (KW, FF), 1.0, 6.0, ((1, 4),), jnp.float32),
    }


root_half = 0.7071067811865476
density_norm = 0.3989422804014327


def causal_mix(gate_rows, taps):
    width = taps.shape[0]
    length = gate_rows.shape[0]
    padded = jnp.pad(gate_rows.astype(jnp.float32), ((width - 1, 0), (0, 0)))
    mixed_pre = jnp.zeros((length, gate_rows.shape[1]), jnp.float32)
    for j in range(width):
        mixed_pre = mixed_pre + padded[j:j + length] * taps[j]
    return mixed_pre, padded


def gelu_slope(mixed_pre):
    return 0.5 * (1.0 + lax.erf(mixed_pre * root_half)) + mixed_pre * jnp.exp(-0.5 * mixed_pre * mixed_pre) * density_norm


def back_mix(slope_rows, taps, padded):
    width = taps.shape[0]
    length = slope_rows.shape[0]
    grown = jnp.pad(slope_rows, ((0, width - 1), (0, 0)))
    d_gate = jnp.zeros(slope_rows.shape, jnp.float32)
    for j in range(width):
        d_gate = d_gate + grown[width - 1 - j:width - 1 - j + length] * taps[j]
    tap_terms = jnp.stack([jnp.sum(slope_rows * padded[j:j + length], axis=0) for j in range(width)])
    return d_gate, tap_terms


def reference(x_late, x_early, w_gate, w_value, conv_taps, grad_hidden, sum_gate, sum_value, sum_taps):
    count_seq = TOKENS // SEQ_LEN
    columns = FF // N_TP
    factor = TOKENS ** -0.5

    def project(x_rows):
        gate_rows = jnp.dot(x_rows, w_gate, preferred_element_type=jnp.float32).astype(jnp.bfloat16)
        value_rows = jnp.dot(x_rows, w_value, preferred_element_type=jnp.float32).astype(jnp.bfloat16)
        return gate_rows, value_rows

    def forward_one(x_rows):
        gate_rows, value_rows = project(x_rows)
        mixed_pre, padded = causal_mix(gate_rows, conv_taps)
        return (jax.nn.gelu(mixed_pre, approximate=False) * value_rows.astype(jnp.float32)).astype(jnp.bfloat16)

    hidden = lax.map(forward_one, x_late.reshape(count_seq, SEQ_LEN, D)).reshape(TOKENS, FF)

    def backward_one(carry, inputs):
        grad_g, grad_v, grad_t = carry
        x_rows, upstream = inputs
        gate_rows, value_rows = project(x_rows)
        mixed_pre, padded = causal_mix(gate_rows, conv_taps)
        upstream_f = upstream.astype(jnp.float32)
        slope_rows = upstream_f * value_rows.astype(jnp.float32) * gelu_slope(mixed_pre)
        d_value = (upstream_f * jax.nn.gelu(mixed_pre, approximate=False)).astype(jnp.bfloat16)
        d_gate_f, tap_terms = back_mix(slope_rows, conv_taps, padded)
        d_gate = d_gate_f.astype(jnp.bfloat16)
        grad_g = grad_g + jnp.dot(x_rows.T, d_gate, preferred_element_type=jnp.float32)
        grad_v = grad_v + jnp.dot(x_rows.T, d_value, preferred_element_type=jnp.float32)
        grad_t = grad_t + tap_terms
        total = jnp.zeros((SEQ_LEN, D), jnp.float32)
        for block in range(N_TP):
            first = block * columns
            part = jnp.dot(d_gate[:, first:first + columns], w_gate[:, first:first + columns].T, preferred_element_type=jnp.float32)
            part = part + jnp.dot(d_value[:, first:first + columns], w_value[:, first:first + columns].T, preferred_element_type=jnp.float32)
            rounded = lax.optimization_barrier(part.astype(jnp.bfloat16))
            total = total + rounded.astype(jnp.float32)
        return (grad_g, grad_v, grad_t), total.astype(jnp.bfloat16)

    start = (jnp.zeros((D, FF), jnp.float32), jnp.zeros((D, FF), jnp.float32), jnp.zeros((KW, FF), jnp.float32))
    inputs = (x_early.reshape(count_seq, SEQ_LEN, D), grad_hidden.reshape(count_seq, SEQ_LEN, FF))
    sums, grads = lax.scan(backward_one, start, inputs)
    grad_g, grad_v, grad_t = sums
    return (hidden, grads.reshape(TOKENS, D), sum_gate + factor * grad_g,
            sum_value + factor * grad_v, sum_taps + factor * grad_t)
```

```python
import functools
import math

import jax
import jax.numpy as jnp
from jax import lax
from jax.experimental import pallas as pl
from jax.experimental.pallas import tpu as pltpu
from jax.sharding import PartitionSpec as P

root_half = 0.7071067811865476
density_norm = 0.3989422804014327
MESH = pl.DeviceIdType.MESH
LANE = 128
LEAD = 2


def kernel(n, tp_n, factor, *refs):
    x_late, x_early, w_gate, w_value, conv, grad_hidden = refs[:6]
    hidden, grad_early, gate_total, value_total, taps_total = refs[6:11]
    (
        strip, late_rows, early_rows, flipped, cots, upstream, out_stage, wire, part_got,
        up_got, down_got, fin_got, partial, partial_got, taps_own, taps_got, conv_got,
    ) = refs[11:28]
    (
        w_out, w_in, up_out, up_in, down_out, down_in, share_out, share_in, u_out, u_in,
        h_out, h_in, q_out, q_in, z_out, zup_in, zdown_in, f_out, f_in, late_out, late_in,
        early_out, early_in, p_out, p_in, t_out, t_in, c_out, c_in,
    ) = refs[28:]
    depth, half = n // 2, tp_n // 2
    rows = gate_total.shape[0]
    columns = gate_total.shape[1]
    strips = columns // LANE
    tokens, width = early_rows.shape
    piece = x_early.shape[0]
    taps_count = conv.shape[0]
    lag = depth + LEAD
    me, tp = lax.axis_index("fs"), lax.axis_index("tp")
    z, y = lax.div(me, 2), lax.rem(me, 2)
    x, c = lax.div(tp, 2), lax.rem(tp, 2)
    same = c == y
    other = jnp.logical_not(same)
    role_fs, role_tp = z * 2 + c, x * 2 + y
    twin = {"fs": role_fs, "tp": role_tp}
    partner = {"fs": me, "tp": x * 2 + 1 - c}
    above, below = {"fs": me + 2, "tp": tp}, {"fs": me - 2, "tp": tp}
    has_up, has_down = z + 1 < depth, z > 0

    def send(src, dst, out_sem, in_sem, to):
        return pltpu.make_async_remote_copy(
            src_ref=src, dst_ref=dst, send_sem=out_sem, recv_sem=in_sem,
            device_id=to, device_id_type=MESH,
        )

    def landed(dst, sem):
        pltpu.make_async_copy(dst, dst, sem).wait()

    def lanes(s):
        return pl.ds(pl.multiple_of(s * LANE, LANE), LANE)

    def block(zz, cc):
        return pl.ds(pl.multiple_of((zz * 2 + cc) * rows, rows), rows)

    def own_slot(s, zz, cc):
        return strip.at[s, block(zz, cc)]

    barrier = pltpu.get_barrier_semaphore()

    def hail(i, _):
        j = lax.rem(me * 2 + c + i, 2 * n)
        pl.semaphore_signal(
            barrier, inc=1, device_id={"fs": lax.div(j, 2), "tp": x * 2 + lax.rem(j, 2)},
            device_id_type=MESH,
        )
        return 0

    lax.fori_loop(1, 2 * n, hail, 0)
    for dx in range(1, half):
        for yy in range(2):
            for cc in range(2):
                pl.semaphore_signal(
                    barrier, inc=1,
                    device_id={"fs": z * 2 + yy, "tp": lax.rem(x + dx, half) * 2 + cc},
                    device_id_type=MESH,
                )
    pl.semaphore_wait(barrier, 2 * n - 1 + 4 * (half - 1))

    def weights_away(s, there):
        for source, at in ((w_gate, 0), (w_value, LANE)):
            src = source.at[:, lanes(s)]
            dst = strip.at[s, block(z, y), pl.ds(at, LANE)]
            if there:
                send(src, dst, w_out.at[s], w_in.at[s], twin).start()
            else:
                pltpu.make_async_copy(src, dst, w_in.at[s]).start()

    def weights_first(first, last):
        def body(s, _):
            pl.when(same)(lambda: weights_away(s, False))
            pl.when(other)(lambda: weights_away(s, True))
            return 0

        lax.fori_loop(first, last, body, 0)

    def upstream_copy(s):
        return send(grad_hidden.at[:, lanes(s)], upstream.at[s], u_out.at[s], u_in.at[s], twin)

    def upstream_first(s, _):
        @pl.when(same)
        def _():
            pltpu.make_async_copy(grad_hidden.at[:, lanes(s)], upstream.at[s], u_in.at[s]).start()

        pl.when(other)(lambda: upstream_copy(s).start())
        return 0

    def token_copies(source, into, out_sem, in_sem):
        copies = []
        for yy in range(2):
            for dx in range(half):
                xx = lax.rem(x + dx, half)
                to = {"fs": z * 2 + yy, "tp": xx * 2 + y}
                dst = into.at[pl.ds(pl.multiple_of(tp * piece, piece), piece)]
                mine = jnp.logical_and(same, yy == y) if dx == 0 else None
                copies.append((mine, source, dst, out_sem.at[yy * half + dx], in_sem.at[tp], to))
        return copies

    def tokens_start(copies):
        for mine, src, dst, out_sem, in_sem, to in copies:
            if mine is None:
                send(src, dst, out_sem, in_sem, to).start()
            else:
                pl.when(mine)(lambda: pltpu.make_async_copy(src, dst, in_sem).start())
                pl.when(jnp.logical_not(mine))(lambda: send(src, dst, out_sem, in_sem, to).start())

    def tokens_sent(copies):
        for mine, src, dst, out_sem, in_sem, to in copies:
            if mine is None:
                send(src, dst, out_sem, in_sem, to).wait_send()
            else:
                pl.when(jnp.logical_not(mine))(lambda: send(src, dst, out_sem, in_sem, to).wait_send())

    def tokens_here(into, in_sem):
        for t in range(tp_n):
            landed(into.at[pl.ds(t * piece, piece)], in_sem.at[t])

    early_copies = token_copies(x_early, early_rows, early_out, early_in)
    late_copies = token_copies(x_late, late_rows, late_out, late_in)
    first = min(3, strips)
    weights_first(0, first)
    conv_copy = send(conv, conv_got, c_out, c_in, partner)
    conv_copy.start()
    tokens_start(early_copies)
    weights_first(first, strips)
    lax.fori_loop(0, strips, upstream_first, 0)
    tokens_start(late_copies)

    def up(s, k):
        at = own_slot(s, z - k, c)
        return send(at, at, up_out.at[s, k], up_in.at[s, k], above)

    def down(s, k):
        at = own_slot(s, z + k, c)
        return send(at, at, down_out.at[s, k], down_in.at[s, k], below)

    def share(s, zz):
        at = own_slot(s, zz, c)
        return send(at, at, share_out.at[s, zz], share_in.at[s, zz], partner)

    def spread(s):
        landed(own_slot(s, z, c), w_in.at[s])
        pl.when(has_up)(lambda: up(s, 0).start())
        pl.when(has_down)(lambda: down(s, 0).start())
        share(s, z).start()

    def hop(s, k):
        @pl.when(z - 1 - k >= 0)
        def _():
            landed(own_slot(s, z - 1 - k, c), up_in.at[s, k])
            pl.when(has_up)(lambda: up(s, k + 1).start())
            share(s, z - 1 - k).start()

        @pl.when(z + 1 + k < depth)
        def _():
            landed(own_slot(s, z + 1 + k, c), down_in.at[s, k])
            pl.when(has_down)(lambda: down(s, k + 1).start())
            share(s, z + 1 + k).start()

    def gathered(s):
        def body(zz, _):
            landed(own_slot(s, zz, 1 - c), share_in.at[s, zz])
            return 0

        lax.fori_loop(0, depth, body, 0)

    def taps_of(s):
        got = jnp.where(same, conv[:, lanes(s)], conv_got[:, lanes(s)])
        return [got[j : j + 1] for j in range(taps_count)]

    def mix(gate, taps):
        position = lax.broadcasted_iota(jnp.int32, gate.shape, 0)
        moved = []
        for j in range(taps_count):
            delay = taps_count - 1 - j
            if delay == 0:
                moved.append(gate)
            else:
                moved.append(jnp.where(position >= delay, pltpu.roll(gate, delay, 0), 0.0))
        pre = moved[0] * taps[0]
        for j in range(1, taps_count):
            pre = pre + moved[j] * taps[j]
        return pre, moved

    def project(source, s):
        both = jnp.dot(source[...], strip[s], preferred_element_type=jnp.float32)
        both = both.astype(jnp.bfloat16).astype(jnp.float32)
        return both[:, :LANE], both[:, LANE:]

    def backward(s):
        landed(upstream.at[s], u_in.at[s])
        gate, value = project(early_rows, s)
        taps = taps_of(s)
        pre, moved = mix(gate, taps)
        cdf = 0.5 * (1.0 + lax.erf(pre * root_half))
        bend = cdf + pre * jnp.exp(-0.5 * pre * pre) * density_norm
        grad = upstream[s].astype(jnp.float32)
        cots[s, :, LANE:] = (grad * (pre * cdf)).astype(cots.dtype)
        slope = grad * value * bend
        for j in range(taps_count):
            taps_own[pl.ds(j, 1), lanes(s)] = jnp.sum(slope * moved[j], axis=0, keepdims=True)
        position = lax.broadcasted_iota(jnp.int32, slope.shape, 0)
        d_gate = slope * taps[taps_count - 1]
        for j in range(taps_count - 1):
            ahead = taps_count - 1 - j
            later = jnp.where(position < tokens - ahead, pltpu.roll(slope, tokens - ahead, 0), 0.0)
            d_gate = d_gate + later * taps[j]
        cots[s, :, :LANE] = d_gate.astype(cots.dtype)

    def term(s, zz, cc):
        return factor * jnp.dot(
            flipped[block(zz, cc), :], cots[s], preferred_element_type=jnp.float32
        )

    def to_partner(s):
        slot = lax.rem(s, 2)
        return send(wire.at[slot], part_got.at[s], q_out.at[slot], q_in.at[s], partner)

    def terms_away(s):
        slot = lax.rem(s, 2)
        pl.when(s >= 2)(lambda: to_partner(s - 2).wait_send())

        def body(zz, _):
            wire[slot, zz] = term(s, zz, 1 - c).astype(wire.dtype)
            return 0

        lax.fori_loop(0, depth, body, 0)
        to_partner(s).start()

    def terms_here(s):
        landed(part_got.at[s], q_in.at[s])

        def body(zz, _):
            value = term(s, zz, c) + part_got[s, zz].astype(jnp.float32)
            part_got[s, zz] = value.astype(part_got.dtype)
            return 0

        lax.fori_loop(0, depth, body, 0)

    def hidden_copy(s, there):
        slot = lax.rem(s, 2)
        src, dst = out_stage.at[slot], hidden.at[:, lanes(s)]
        if there:
            return send(src, dst, h_out.at[slot], h_in.at[s], twin)
        return pltpu.make_async_copy(src, dst, h_out.at[slot])

    def hidden_sent(s):
        pl.when(other)(lambda: hidden_copy(s, True).wait_send())
        pl.when(same)(lambda: hidden_copy(s, False).wait())

    def forward(s):
        slot = lax.rem(s, 2)
        pl.when(s >= 2)(lambda: hidden_sent(s - 2))
        gate, value = project(late_rows, s)
        pre, _ = mix(gate, taps_of(s))
        active = 0.5 * pre * (1.0 + lax.erf(pre * root_half))
        out_stage[slot] = (active * value).astype(out_stage.dtype)
        pl.when(other)(lambda: hidden_copy(s, True).start())
        pl.when(same)(lambda: hidden_copy(s, False).start())

    def along(s, zz, away, upward):
        got, sem, to = (up_got, zup_in, above) if upward else (down_got, zdown_in, below)
        return send(part_got.at[s, zz], got.at[s, away - 1], z_out.at[s, zz], sem.at[s, away - 1], to)

    def pass_on(s, away, upward):
        zz = z + away if upward else z - away
        got, sem = (up_got, zup_in) if upward else (down_got, zdown_in)

        @pl.when(zz < depth if upward else zz >= 0)
        def _():
            if away < depth - 1:

                @pl.when(has_down if upward else has_up)
                def _():
                    landed(got.at[s, away], sem.at[s, away])
                    value = part_got[s, zz].astype(jnp.float32) + got[s, away].astype(jnp.float32)
                    part_got[s, zz] = value.astype(part_got.dtype)

            along(s, zz, away, upward).start()

    def fin(s):
        return send(part_got.at[s, z], fin_got.at[s], f_out.at[s], f_in.at[s], twin)

    def put_total(s, value):
        gate_total[:, lanes(s)] = value[:, :LANE]
        value_total[:, lanes(s)] = value[:, LANE:]

    def finish(s):
        pl.when(has_down)(lambda: landed(up_got.at[s, 0], zup_in.at[s, 0]))
        pl.when(has_up)(lambda: landed(down_got.at[s, 0], zdown_in.at[s, 0]))

        def settle(value):
            pl.when(same)(lambda: put_total(s, value))

            @pl.when(other)
            def _():
                part_got[s, z] = value.astype(part_got.dtype)

        def total(refs_):
            value = part_got[s, z].astype(jnp.float32)
            for ref in refs_:
                value = value + ref[s, 0].astype(jnp.float32)
            settle(value)

        pl.when(jnp.logical_not(has_down))(lambda: total([down_got]))
        pl.when(jnp.logical_not(has_up))(lambda: total([up_got]))
        pl.when(jnp.logical_and(has_up, has_down))(lambda: total([up_got, down_got]))
        pl.when(other)(lambda: fin(s).start())

    def accept(s):
        @pl.when(other)
        def _():
            landed(fin_got.at[s], f_in.at[s])
            put_total(s, fin_got[s].astype(jnp.float32))

    def input_grad():
        contract = (((1,), (1,)), ((), ()))
        wide = 2 * LANE

        def body(b, _):
            at = pl.ds(pl.multiple_of(b * wide, wide), wide)
            total = jnp.zeros((tokens, wide), jnp.float32)
            for s in range(strips):
                total = total + lax.dot_general(
                    cots[s], strip[s, at, :], contract, preferred_element_type=jnp.float32
                )
            partial[:, at] = total.astype(partial.dtype)
            return 0

        lax.fori_loop(0, width // wide, body, 0)

    def partial_rows(t):
        return partial.at[pl.ds(pl.multiple_of(t * piece, piece), piece)]

    def partial_copies(fn_there, fn_here):
        for i in range(1, tp_n + 1):
            t = lax.rem(tp + i, tp_n)
            copy = send(
                partial_rows(t), partial_got.at[role_tp], p_out.at[t], p_in.at[role_tp],
                {"fs": role_fs, "tp": t},
            )
            here = jnp.logical_and(same, t == tp)
            pl.when(jnp.logical_not(here))(lambda: fn_there(copy))
            if fn_here is not None:
                pl.when(here)(
                    lambda: fn_here(
                        pltpu.make_async_copy(partial_rows(t), partial_got.at[role_tp], p_in.at[role_tp])
                    )
                )

    def taps_copies(fn_there, fn_here):
        def body(f, _):
            copy = send(
                taps_own, taps_got.at[role_fs], t_out.at[f], t_in.at[role_fs],
                {"fs": f, "tp": role_tp},
            )
            here = jnp.logical_and(same, f == me)
            pl.when(jnp.logical_not(here))(lambda: fn_there(copy))
            if fn_here is not None:
                pl.when(here)(
                    lambda: fn_here(pltpu.make_async_copy(taps_own, taps_got.at[role_fs], t_in.at[role_fs]))
                )
            return 0

        lax.fori_loop(0, n, body, 0)

    def guarded(s, work):
        pl.when(jnp.logical_and(s >= 0, s < strips))(lambda: work(s))

    def prepare():
        tokens_here(early_rows, early_in)
        conv_copy.wait_recv()
        taps_own[...] = jnp.zeros(taps_own.shape, jnp.float32)
        wide = 2 * LANE
        for b in range(width // wide):
            flipped[b * wide : (b + 1) * wide, :] = early_rows[:, b * wide : (b + 1) * wide].T

    def strip_work(s):
        pl.when(s == 0)(prepare)
        gathered(s)
        backward(s)
        terms_away(s)
        pl.when(s == 0)(lambda: tokens_here(late_rows, late_in))
        forward(s)
        terms_here(s)
        for upward in (True, False):
            pass_on(s, depth - 1, upward)

    def step(t, _):
        guarded(t, spread)
        for k in range(depth - 1):
            guarded(t - 1 - k, lambda s, k=k: hop(s, k))
        guarded(t - lag, strip_work)

        @pl.when(t == strips + lag - 1)
        def _():
            taps_copies(lambda copy: copy.start(), lambda copy: copy.start())
            input_grad()
            partial_copies(lambda copy: copy.start(), lambda copy: copy.start())

        for away in range(depth - 2, 0, -1):
            for upward in (True, False):
                guarded(t - lag - (depth - 1 - away), lambda s: pass_on(s, away, upward))
        guarded(t - lag - (depth - 1), finish)
        guarded(t - lag - depth, accept)
        return 0

    lax.fori_loop(0, strips + lag + depth, step, 0)

    def taps_arrive(f, _):
        landed(taps_got.at[f], t_in.at[f])
        return 0

    lax.fori_loop(0, n, taps_arrive, 0)
    sum_of = taps_got[0]
    for i in range(1, n):
        sum_of = sum_of + taps_got[i]
    taps_total[...] = factor * sum_of

    for t in range(tp_n):
        landed(partial_got.at[t], p_in.at[t])
    total = partial_got[0].astype(jnp.float32)
    for t in range(1, tp_n):
        total = total + partial_got[t].astype(jnp.float32)
    grad_early[...] = total.astype(grad_early.dtype)

    conv_copy.wait_send()
    tokens_sent(early_copies)
    tokens_sent(late_copies)
    taps_copies(lambda copy: copy.wait_send(), None)
    partial_copies(lambda copy: copy.wait_send(), None)
    for s in range(max(0, strips - 2), strips):
        to_partner(s).wait_send()
        hidden_sent(s)

    def drain(s, _):
        @pl.when(other)
        def _():
            landed(own_slot(s, z, c), w_out.at[s])
            upstream_copy(s).wait_send()
            hidden_copy(s, True).wait_recv()
            fin(s).wait_send()

        for k in range(depth - 1):
            pl.when(jnp.logical_and(has_up, z - k >= 0))(lambda k=k: up(s, k).wait_send())
            pl.when(jnp.logical_and(has_down, z + k < depth))(lambda k=k: down(s, k).wait_send())
            away = k + 1
            pl.when(z + away < depth)(lambda away=away: along(s, z + away, away, True).wait_send())
            pl.when(z - away >= 0)(lambda away=away: along(s, z - away, away, False).wait_send())
        lax.fori_loop(0, depth, lambda zz, _: (share(s, zz).wait_send(), 0)[1], 0)
        return 0

    lax.fori_loop(0, strips, drain, 0)


def shards(x_late, x_early, w_gate, w_value, conv_taps, grad_hidden, sum_gate, sum_value, sum_taps):
    n, tp_n = lax.axis_size("fs"), lax.axis_size("tp")
    piece, width = x_early.shape
    rows, columns = w_gate.shape
    tokens = piece * tp_n
    strips, depth = columns // LANE, n // 2
    factor = 1.0 / math.sqrt(tokens * n)
    bf16, f32 = x_early.dtype, jnp.float32
    sems = pltpu.SemaphoreType.DMA
    vmem = pl.BlockSpec(memory_space=pltpu.VMEM)
    hbm = pl.BlockSpec(memory_space=pl.ANY)
    taps_shape = (8, columns)
    hops = depth - 1
    hidden, grad_early, gate_total, value_total, taps_total = pl.pallas_call(
        functools.partial(kernel, n, tp_n, factor),
        out_shape=(
            jax.ShapeDtypeStruct((tokens, columns), bf16),
            jax.ShapeDtypeStruct((piece, width), bf16),
            jax.ShapeDtypeStruct((rows, columns), f32),
            jax.ShapeDtypeStruct((rows, columns), f32),
            jax.ShapeDtypeStruct(taps_shape, f32),
        ),
        in_specs=[hbm] * 4 + [vmem] + [hbm],
        out_specs=(hbm,) + (vmem,) * 4,
        scratch_shapes=[
            pltpu.VMEM((strips, n * rows, 2 * LANE), bf16),
            pltpu.VMEM((tokens, width), bf16),
            pltpu.VMEM((tokens, width), bf16),
            pltpu.VMEM((width, tokens), bf16),
            pltpu.VMEM((strips, tokens, 2 * LANE), bf16),
            pltpu.VMEM((strips, tokens, LANE), bf16),
            pltpu.VMEM((2, tokens, LANE), bf16),
            pltpu.VMEM((2, depth, rows, 2 * LANE), bf16),
            pltpu.VMEM((strips, depth, rows, 2 * LANE), bf16),
            pltpu.VMEM((strips, hops, rows, 2 * LANE), bf16),
            pltpu.VMEM((strips, hops, rows, 2 * LANE), bf16),
            pltpu.VMEM((strips, rows, 2 * LANE), bf16),
            pltpu.VMEM((tokens, width), bf16),
            pltpu.VMEM((tp_n, piece, width), bf16),
            pltpu.VMEM(taps_shape, f32),
            pltpu.VMEM((n,) + taps_shape, f32),
            pltpu.VMEM(conv_taps.shape, f32),
        ]
        + [sems((strips,))] * 2
        + [sems((strips, hops))] * 4
        + [sems((strips, depth))] * 2
        + [sems((strips,))] * 2
        + [sems((2,)), sems((strips,))]
        + [sems((2,)), sems((strips,))]
        + [sems((strips, depth)), sems((strips, hops)), sems((strips, hops))]
        + [sems((strips,))] * 2
        + [sems((tp_n,))] * 6
        + [sems((n,))] * 2
        + [sems, sems],
        compiler_params=pltpu.CompilerParams(
            collective_id=0, has_side_effects=True, vmem_limit_bytes=67043328
        ),
        name="layer",
    )(x_late, x_early, w_gate, w_value, conv_taps, grad_hidden)
    return (
        hidden,
        grad_early,
        sum_gate + gate_total,
        sum_value + value_total,
        sum_taps + taps_total[: conv_taps.shape[0]],
    )


def solution(mesh):
    placed = (
        P(("fs", "tp"), None),
        P(("fs", "tp"), None),
        P("fs", "tp"),
        P("fs", "tp"),
        P(None, "tp"),
        P("fs", "tp"),
        P("fs", "tp"),
        P("fs", "tp"),
        P(None, "tp"),
    )
    return jax.shard_map(
        shards,
        mesh=mesh,
        in_specs=placed,
        out_specs=(
            P("fs", "tp"),
            P(("fs", "tp"), None),
            P("fs", "tp"),
            P("fs", "tp"),
            P(None, "tp"),
        ),
        check_vma=False,
    )
```

```python
import functools
import math

import jax
import jax.numpy as jnp
from jax import lax
from jax.experimental import pallas as pl
from jax.experimental.pallas import tpu as pltpu
from jax.sharding import PartitionSpec as P

root_half = 0.7071067811865476
density_norm = 0.3989422804014327
MESH = pl.DeviceIdType.MESH
LANE = 128
HOP = 2
BEHIND = 5
DELAY = 1
FLUSH = 1
PER_STEP = 2
GROUPS = (7, 3)
TURN = 2


def kernel(n, tp_n, factor, *refs):
    x_late, x_early, w_gate, w_value, conv, grad_hidden, sum_gate, sum_value, sum_taps = refs[:9]
    hidden, grad_early, new_gate, new_value, new_taps = refs[9:14]
    (
        strip, late_rows, early_rows, flipped, cots, upstream, out_stage, wire, part_got,
        up_got, down_got, fin_got, partial, partial_got, taps_own, taps_got, conv_got, ahead,
        gate_total, value_total,
    ) = refs[14:34]
    (
        w_out, w_in, up_out, up_in, down_out, down_in, share_out, share_in, u_out, u_in,
        h_out, h_in, q_out, q_in, z_out, zup_in, zdown_in, f_out, f_in, late_out, late_in,
        early_out, early_in, late_pass, early_pass, p_out, p_in, t_out, t_in, c_out, c_in,
        sums_in, sums_out,
    ) = refs[34:]
    depth, half = n // 2, tp_n // 2
    rows, columns = gate_total.shape
    strips = columns // LANE
    tokens, width = early_rows.shape
    piece = x_early.shape[0]
    taps_count = conv.shape[0]
    lag = HOP + depth - 1
    late_at = lag + BEHIND
    last_hop = lag + depth - 2
    flush = max(strips + lag - FLUSH, last_hop)
    parts = early_in.shape[1]
    part = piece // parts
    groups = [0] + [strips - k for k in GROUPS if strips > k] + [strips]
    me, tp = lax.axis_index("fs"), lax.axis_index("tp")
    z, y = lax.div(me, 2), lax.rem(me, 2)
    x, c = lax.div(tp, 2), lax.rem(tp, 2)
    same = c == y
    other = jnp.logical_not(same)
    role_fs, role_tp = z * 2 + c, x * 2 + y
    twin = {"fs": role_fs, "tp": role_tp}
    partner = {"fs": me, "tp": x * 2 + 1 - c}
    above, below = {"fs": me + 2, "tp": tp}, {"fs": me - 2, "tp": tp}
    has_up, has_down = z + 1 < depth, z > 0

    def send(src, dst, out_sem, in_sem, to):
        return pltpu.make_async_remote_copy(
            src_ref=src, dst_ref=dst, send_sem=out_sem, recv_sem=in_sem,
            device_id=to, device_id_type=MESH,
        )

    def landed(dst, sem):
        pltpu.make_async_copy(dst, dst, sem).wait()

    def lanes(s):
        return pl.ds(pl.multiple_of(s * LANE, LANE), LANE)

    def block(zz, cc):
        return pl.ds(pl.multiple_of((zz * 2 + cc) * rows, rows), rows)

    def own_slot(s, zz, cc):
        return strip.at[s, block(zz, cc)]

    barrier = pltpu.get_barrier_semaphore()

    def hail(i, _):
        j = lax.rem(me * 2 + c + i, 2 * n)
        pl.semaphore_signal(
            barrier, inc=1, device_id={"fs": lax.div(j, 2), "tp": x * 2 + lax.rem(j, 2)},
            device_id_type=MESH,
        )
        return 0

    lax.fori_loop(1, 2 * n, hail, 0)
    for dx in range(1, half):
        for yy in range(2):
            for cc in range(2):
                pl.semaphore_signal(
                    barrier, inc=1,
                    device_id={"fs": z * 2 + yy, "tp": lax.rem(x + dx, half) * 2 + cc},
                    device_id_type=MESH,
                )
    pl.semaphore_wait(barrier, 2 * n - 1 + 4 * (half - 1))

    def weights_away(s, there):
        for source, at in ((w_gate, 0), (w_value, LANE)):
            src = source.at[:, lanes(s)]
            dst = strip.at[s, block(z, y), pl.ds(at, LANE)]
            if there:
                send(src, dst, w_out.at[s], w_in.at[s], twin).start()
            else:
                pltpu.make_async_copy(src, dst, w_in.at[s]).start()

    def weights_first(first, last):
        def body(s, _):
            pl.when(same)(lambda: weights_away(s, False))
            pl.when(other)(lambda: weights_away(s, True))
            return 0

        lax.fori_loop(first, last, body, 0)

    def upstream_copy(s):
        return send(grad_hidden.at[:, lanes(s)], upstream.at[s], u_out.at[s], u_in.at[s], twin)

    def upstream_first(s, _):
        @pl.when(same)
        def _():
            pltpu.make_async_copy(grad_hidden.at[:, lanes(s)], upstream.at[s], u_in.at[s]).start()

        pl.when(other)(lambda: upstream_copy(s).start())
        return 0

    def token_part(into, t, q):
        return into.at[pl.ds(pl.multiple_of(t * piece + q * part, part), part)]

    def token_copies(source, into, out_sem, in_sem, q):
        copies = []
        for i, (dx, yy) in enumerate([(0, 1 - y)] + [(dx, y) for dx in range(1, half)] + [(0, y)]):
            to = {"fs": z * 2 + yy, "tp": lax.rem(x + dx, half) * 2 + y}
            mine = same if i == half else None
            src = source.at[pl.ds(q * part, part)]
            copies.append((mine, src, token_part(into, tp, q), out_sem.at[i, q], in_sem.at[tp, q], to))
        return copies

    def tokens_start(copies):
        for mine, src, dst, out_sem, in_sem, to in copies:
            if mine is None:
                send(src, dst, out_sem, in_sem, to).start()
            else:
                pl.when(mine)(lambda: pltpu.make_async_copy(src, dst, in_sem).start())
                pl.when(jnp.logical_not(mine))(lambda: send(src, dst, out_sem, in_sem, to).start())

    def tokens_sent(copies):
        for mine, src, dst, out_sem, in_sem, to in copies:
            if mine is None:
                send(src, dst, out_sem, in_sem, to).wait_send()
            else:
                pl.when(jnp.logical_not(mine))(lambda: send(src, dst, out_sem, in_sem, to).wait_send())

    def turn(into, in_sem, pass_sem, cc, dx, q):
        t = x * 2 + cc
        at = token_part(into, t, q)
        to = {"fs": me, "tp": lax.rem(x + dx, half) * 2 + c}
        return send(at, at, pass_sem.at[cc * half + dx, q], in_sem.at[t, q], to)

    def tokens_turn(into, in_sem, pass_sem, q):
        @pl.when(other)
        def _():
            for cc in range(2):
                landed(token_part(into, x * 2 + cc, q), in_sem.at[x * 2 + cc, q])
                for dx in range(1, half):
                    turn(into, in_sem, pass_sem, cc, dx, q).start()

    def turned(into, in_sem, pass_sem):
        @pl.when(other)
        def _():
            for q in range(parts):
                for dx in range(1, half):
                    for cc in range(2):
                        turn(into, in_sem, pass_sem, cc, dx, q).wait_send()

    def tokens_here(into, in_sem):
        for t in range(tp_n):

            @pl.when(jnp.logical_or(same, x != t // 2))
            def _():
                for q in range(parts):
                    landed(token_part(into, t, q), in_sem.at[t, q])

    early_copies = [token_copies(x_early, early_rows, early_out, early_in, q) for q in range(parts)]
    late_copies = [token_copies(x_late, late_rows, late_out, late_in, q) for q in range(parts)]
    first = min(2, strips)
    weights_first(0, first)
    conv_copy = send(conv, conv_got, c_out, c_in, partner)
    conv_copy.start()
    for q in range(parts):
        tokens_start(early_copies[q])
        weights_first(min(first + q, strips), min(first + q + 1, strips))
    soon = min(first + parts, strips)
    head = min(4, strips)

    def second_wave():
        def body(s, _):
            pl.when(s < head)(lambda: (upstream_first(s, 0), None)[1])
            at = soon + 2 * s
            for i in range(2):
                pl.when(at + i < strips)(lambda: weights_first(at + i, at + i + 1))
            return 0

        lax.fori_loop(0, max(head, -(-(strips - soon) // 2)), body, 0)

    def third_wave():
        for q in range(parts):
            tokens_start(late_copies[q])
            lax.fori_loop(min(head + q, strips), min(head + q + 1, strips), upstream_first, 0)
        lax.fori_loop(min(head + parts, strips), strips, upstream_first, 0)

    def up(s, k):
        at = own_slot(s, z - k, c)
        return send(at, at, up_out.at[s, k], up_in.at[s, k], above)

    def down(s, k):
        at = own_slot(s, z + k, c)
        return send(at, at, down_out.at[s, k], down_in.at[s, k], below)

    def share(s, zz):
        at = own_slot(s, zz, c)
        return send(at, at, share_out.at[s, zz], share_in.at[s, zz], partner)

    def spread(s):
        landed(own_slot(s, z, c), w_in.at[s])
        pl.when(has_up)(lambda: up(s, 0).start())
        pl.when(has_down)(lambda: down(s, 0).start())
        share(s, z).start()

    def hop(s, k):
        @pl.when(z - 1 - k >= 0)
        def _():
            landed(own_slot(s, z - 1 - k, c), up_in.at[s, k])
            pl.when(has_up)(lambda: up(s, k + 1).start())
            share(s, z - 1 - k).start()

        @pl.when(z + 1 + k < depth)
        def _():
            landed(own_slot(s, z + 1 + k, c), down_in.at[s, k])
            pl.when(has_down)(lambda: down(s, k + 1).start())
            share(s, z + 1 + k).start()

    def gathered(s):
        def body(zz, _):
            landed(own_slot(s, zz, 1 - c), share_in.at[s, zz])
            return 0

        lax.fori_loop(0, depth, body, 0)

    def taps_of(s):
        got = jnp.where(same, conv[:, lanes(s)], conv_got[:, lanes(s)])
        return [got[j : j + 1] for j in range(taps_count)]

    def mix(gate, taps):
        position = lax.broadcasted_iota(jnp.int32, gate.shape, 0)
        moved = []
        for j in range(taps_count):
            delay = taps_count - 1 - j
            if delay == 0:
                moved.append(gate)
            else:
                moved.append(jnp.where(position >= delay, pltpu.roll(gate, delay, 0), 0.0))
        pre = moved[0] * taps[0]
        for j in range(1, taps_count):
            pre = pre + moved[j] * taps[j]
        return pre, moved

    def project(source, s):
        both = jnp.dot(source[...], strip[s], preferred_element_type=jnp.float32)
        both = both.astype(jnp.bfloat16).astype(jnp.float32)
        return both[:, :LANE], both[:, LANE:]

    def backward(s):
        landed(upstream.at[s], u_in.at[s])
        gate, value = project(early_rows, s)
        taps = taps_of(s)
        pre, moved = mix(gate, taps)
        cdf = 0.5 * (1.0 + lax.erf(pre * root_half))
        bend = cdf + pre * jnp.exp(-0.5 * pre * pre) * density_norm
        grad = upstream[s].astype(jnp.float32)
        cots[s, :, LANE:] = (grad * (pre * cdf)).astype(cots.dtype)
        slope = grad * value * bend
        for j in range(taps_count):
            taps_own[pl.ds(j, 1), lanes(s)] = jnp.sum(slope * moved[j], axis=0, keepdims=True)
        position = lax.broadcasted_iota(jnp.int32, slope.shape, 0)
        d_gate = slope * taps[taps_count - 1]
        for j in range(taps_count - 1):
            ahead = taps_count - 1 - j
            later = jnp.where(position < tokens - ahead, pltpu.roll(slope, tokens - ahead, 0), 0.0)
            d_gate = d_gate + later * taps[j]
        cots[s, :, :LANE] = d_gate.astype(cots.dtype)

    def term(s, zz, cc):
        return factor * jnp.dot(
            flipped[block(zz, cc), :], cots[s], preferred_element_type=jnp.float32
        )

    def to_partner(s):
        slot = lax.rem(s, 2)
        return send(wire.at[slot], part_got.at[s], q_out.at[slot], q_in.at[s], partner)

    def terms_away(s):
        slot = lax.rem(s, 2)
        pl.when(s >= 2)(lambda: to_partner(s - 2).wait_send())

        def body(zz, _):
            wire[slot, zz] = term(s, zz, 1 - c).astype(wire.dtype)
            return 0

        lax.fori_loop(0, depth, body, 0)
        to_partner(s).start()

    def terms_here(s):
        landed(part_got.at[s], q_in.at[s])

        def body(zz, _):
            value = term(s, zz, c) + part_got[s, zz].astype(jnp.float32)
            part_got[s, zz] = value.astype(part_got.dtype)
            return 0

        lax.fori_loop(0, depth, body, 0)

    def hidden_copy(s, there):
        slot = lax.rem(s, 2)
        src, dst = out_stage.at[slot], hidden.at[:, lanes(s)]
        if there:
            return send(src, dst, h_out.at[slot], h_in.at[s], twin)
        return pltpu.make_async_copy(src, dst, h_out.at[slot])

    def hidden_sent(s):
        pl.when(other)(lambda: hidden_copy(s, True).wait_send())
        pl.when(same)(lambda: hidden_copy(s, False).wait())

    def forward(s):
        slot = lax.rem(s, 2)
        pl.when(s >= 2)(lambda: hidden_sent(s - 2))
        gate, value = project(late_rows, s)
        pre, _ = mix(gate, taps_of(s))
        active = 0.5 * pre * (1.0 + lax.erf(pre * root_half))
        out_stage[slot] = (active * value).astype(out_stage.dtype)
        pl.when(other)(lambda: hidden_copy(s, True).start())
        pl.when(same)(lambda: hidden_copy(s, False).start())

    def along(s, zz, away, upward):
        got, sem, to = (up_got, zup_in, above) if upward else (down_got, zdown_in, below)
        return send(part_got.at[s, zz], got.at[s, away - 1], z_out.at[s, zz], sem.at[s, away - 1], to)

    def pass_on(s, away, upward):
        zz = z + away if upward else z - away
        inside = zz < depth if upward else zz >= 0
        got, sem = (up_got, zup_in) if upward else (down_got, zdown_in)

        @pl.when(inside)
        def _():
            if away < depth - 1:

                @pl.when(has_down if upward else has_up)
                def _():
                    landed(got.at[s, away], sem.at[s, away])
                    value = part_got[s, zz].astype(jnp.float32) + got[s, away].astype(jnp.float32)
                    part_got[s, zz] = value.astype(part_got.dtype)

            along(s, zz, away, upward).start()

    def fin(s):
        return send(part_got.at[s, z], fin_got.at[s], f_out.at[s], f_in.at[s], twin)

    sums = ((sum_gate, gate_total, new_gate), (sum_value, value_total, new_value))

    def sum_load(i):
        return pltpu.make_async_copy(sums[i][0], sums[i][1], sums_in.at[i])

    def sum_store(i, s):
        at = (slice(None), lanes(s))
        return pltpu.make_async_copy(sums[i][1].at[at], sums[i][2].at[at], sums_out.at[s, i])

    def put_total(s, value):
        gate_total[:, lanes(s)] += value[:, :LANE]
        value_total[:, lanes(s)] += value[:, LANE:]
        for i in range(2):
            sum_store(i, s).start()

    def finish(s):
        pl.when(has_down)(lambda: landed(up_got.at[s, 0], zup_in.at[s, 0]))
        pl.when(has_up)(lambda: landed(down_got.at[s, 0], zdown_in.at[s, 0]))

        def settle(value):
            pl.when(same)(lambda: put_total(s, value))

            @pl.when(other)
            def _():
                part_got[s, z] = value.astype(part_got.dtype)

        def total(refs_):
            value = part_got[s, z].astype(jnp.float32)
            for ref in refs_:
                value = value + ref[s, 0].astype(jnp.float32)
            settle(value)

        pl.when(jnp.logical_not(has_down))(lambda: total([down_got]))
        pl.when(jnp.logical_not(has_up))(lambda: total([up_got]))
        pl.when(jnp.logical_and(has_up, has_down))(lambda: total([up_got, down_got]))
        pl.when(other)(lambda: fin(s).start())

    def accept(s):
        @pl.when(other)
        def _():
            landed(fin_got.at[s], f_in.at[s])
            put_total(s, fin_got[s].astype(jnp.float32))

    wide = 2 * LANE
    blocks = width // wide

    def grad_block(b, first, last):
        at = pl.ds(pl.multiple_of(b * wide, wide), wide)
        total = jnp.zeros((tokens, wide), jnp.float32)
        for s in range(first, last):
            total = total + lax.dot_general(
                cots[s], strip[s, at, :], (((1,), (1,)), ((), ())), preferred_element_type=jnp.float32
            )
        return at, total

    def input_grad_ahead(s):
        for g in range(len(groups) - 2):
            start, end = groups[g + 1], groups[g + 2]
            share_of = -(-blocks // (end - start))

            @pl.when(jnp.logical_and(s >= start, s < end))
            def _():
                first = (s - start) * share_of

                def body(b, _):
                    at, total = grad_block(b, groups[g], start)
                    if g > 0:
                        total = total + ahead[:, at]
                    ahead[:, at] = total
                    return 0

                lax.fori_loop(jnp.minimum(first, blocks), jnp.minimum(first + share_of, blocks), body, 0)

    def input_grad():
        def body(b, _):
            at, total = grad_block(b, groups[-2], strips)
            if len(groups) > 2:
                total = total + ahead[:, at]
            partial[:, at] = total.astype(partial.dtype)
            return 0

        lax.fori_loop(0, blocks, body, 0)

    def partial_rows(t):
        return partial.at[pl.ds(pl.multiple_of(t * piece, piece), piece)]

    def partial_copy(i, fn_there, fn_here):
        t = lax.rem(tp + i, tp_n)
        copy = send(
            partial_rows(t), partial_got.at[role_tp], p_out.at[t], p_in.at[role_tp],
            {"fs": role_fs, "tp": t},
        )
        here = jnp.logical_and(same, t == tp)
        pl.when(jnp.logical_not(here))(lambda: fn_there(copy))
        if fn_here is not None:
            pl.when(here)(
                lambda: fn_here(
                    pltpu.make_async_copy(partial_rows(t), partial_got.at[role_tp], p_in.at[role_tp])
                )
            )

    def taps_copies(fn_there, fn_here):
        def body(f, _):
            copy = send(
                taps_own, taps_got.at[role_fs], t_out.at[f], t_in.at[role_fs],
                {"fs": f, "tp": role_tp},
            )
            here = jnp.logical_and(same, f == me)
            pl.when(jnp.logical_not(here))(lambda: fn_there(copy))
            if fn_here is not None:
                pl.when(here)(
                    lambda: fn_here(pltpu.make_async_copy(taps_own, taps_got.at[role_fs], t_in.at[role_fs]))
                )
            return 0

        lax.fori_loop(0, n, body, 0)

    for i in range(2):
        sum_load(i).start()

    def guarded(s, work):
        pl.when(jnp.logical_and(s >= 0, s < strips))(lambda: (work(s), None)[1])

    def prepare():
        for i in range(2):
            sum_load(i).wait()
        tokens_here(early_rows, early_in)
        conv_copy.wait_recv()
        taps_own[...] = jnp.zeros(taps_own.shape, jnp.float32)
        wide = 2 * LANE
        for b in range(width // wide):
            flipped[b * wide : (b + 1) * wide, :] = early_rows[:, b * wide : (b + 1) * wide].T

    def delayed(t, at, steps, work):
        until = flush + at - last_hop
        pl.when(t < until)(lambda: guarded(t - at - steps, work))

        @pl.when(t == until)
        def _():
            lax.fori_loop(
                jnp.maximum(0, until - at - steps), min(strips, until - at),
                lambda s, _: (work(s), 0)[1], 0,
            )

        pl.when(t >= until)(lambda: guarded(t - at, work))

    def strip_work(s):
        pl.when(s == 0)(prepare)
        gathered(s)
        backward(s)
        terms_away(s)

    def late_work(s):
        pl.when(s == 0)(lambda: tokens_here(late_rows, late_in))
        forward(s)

    def own_work(s):
        terms_here(s)
        for upward in (True, False):
            pass_on(s, depth - 1, upward)
        input_grad_ahead(s)

    def step(t, _):
        guarded(t, spread)
        for k in range(depth - 1):
            guarded(t - HOP - k, lambda s, k=k: hop(s, k))

        for q in range(parts):
            pl.when(t == min(1 + (q + 1) // 2, lag - 1))(
                lambda: tokens_turn(early_rows, early_in, early_pass, q)
            )
            pl.when(t == min(lag + TURN + q, late_at - 1))(
                lambda: tokens_turn(late_rows, late_in, late_pass, q)
            )
        pl.when(t == min(3, lag - 1))(second_wave)
        guarded(t - lag, strip_work)

        for j in range(2):
            guarded(2 * (t - late_at) + j, late_work)
        guarded(t - lag, own_work)
        pl.when(t == lag)(third_wave)

        @pl.when(t == strips + lag - 1)
        def _():
            taps_copies(lambda copy: copy.start(), lambda copy: copy.start())
            input_grad()

        for away in range(depth - 2, 0, -1):
            for upward in (True, False):
                links = z if upward else depth - 1 - z
                delayed(
                    t, lag + depth - 1 - away, DELAY * links, lambda s: pass_on(s, away, upward)
                )
        links = jnp.maximum(jnp.where(has_down, z - 1, 0), jnp.where(has_up, depth - 2 - z, 0))
        delayed(t, last_hop + 1, DELAY * links, finish)
        delayed(t, last_hop + 2, DELAY * links, accept)
        for i in range(tp_n):
            pl.when(t == strips + lag - 1 + i // PER_STEP)(
                lambda: partial_copy(tp_n - i, lambda copy: copy.start(), lambda copy: copy.start())
            )
        return 0

    lax.fori_loop(0, max(strips + lag + max(depth, tp_n), late_at + strips // 2 + 1), step, 0)

    def taps_arrive(f, _):
        landed(taps_got.at[f], t_in.at[f])
        return 0

    lax.fori_loop(0, n, taps_arrive, 0)
    sum_of = taps_got[0]
    for i in range(1, n):
        sum_of = sum_of + taps_got[i]
    new_taps[...] = sum_taps[...] + factor * sum_of[:taps_count]

    for t in range(tp_n):
        landed(partial_got.at[t], p_in.at[t])
    total = partial_got[0].astype(jnp.float32)
    for t in range(1, tp_n):
        total = total + partial_got[t].astype(jnp.float32)
    grad_early[...] = total.astype(grad_early.dtype)

    conv_copy.wait_send()
    for q in range(parts):
        tokens_sent(early_copies[q])
        tokens_sent(late_copies[q])
    turned(early_rows, early_in, early_pass)
    turned(late_rows, late_in, late_pass)
    taps_copies(lambda copy: copy.wait_send(), None)
    for i in range(tp_n):
        partial_copy(i, lambda copy: copy.wait_send(), None)
    for s in range(max(0, strips - 2), strips):
        to_partner(s).wait_send()
        hidden_sent(s)

    def drain(s, _):
        for i in range(2):
            sum_store(i, s).wait()

        @pl.when(other)
        def _():
            landed(own_slot(s, z, c), w_out.at[s])
            upstream_copy(s).wait_send()
            hidden_copy(s, True).wait_recv()
            fin(s).wait_send()

        for k in range(depth - 1):
            pl.when(jnp.logical_and(has_up, z - k >= 0))(lambda k=k: up(s, k).wait_send())
            pl.when(jnp.logical_and(has_down, z + k < depth))(lambda k=k: down(s, k).wait_send())
            away = k + 1
            pl.when(z + away < depth)(lambda away=away: along(s, z + away, away, True).wait_send())
            pl.when(z - away >= 0)(lambda away=away: along(s, z - away, away, False).wait_send())
        lax.fori_loop(0, depth, lambda zz, _: (share(s, zz).wait_send(), 0)[1], 0)
        return 0

    lax.fori_loop(0, strips, drain, 0)


def shards(x_late, x_early, w_gate, w_value, conv_taps, grad_hidden, sum_gate, sum_value, sum_taps):
    n, tp_n = lax.axis_size("fs"), lax.axis_size("tp")
    piece, width = x_early.shape
    rows, columns = w_gate.shape
    tokens = piece * tp_n
    strips, depth = columns // LANE, n // 2
    factor = 1.0 / math.sqrt(tokens * n)
    bf16, f32 = x_early.dtype, jnp.float32
    sems = pltpu.SemaphoreType.DMA
    vmem = pl.BlockSpec(memory_space=pltpu.VMEM)
    hbm = pl.BlockSpec(memory_space=pl.ANY)
    taps_shape = (8, columns)
    hops = depth - 1
    parts = next(q for q in (4, 2, 1) if piece % (16 * q) == 0)
    return pl.pallas_call(
        functools.partial(kernel, n, tp_n, factor),
        out_shape=(
            jax.ShapeDtypeStruct((tokens, columns), bf16),
            jax.ShapeDtypeStruct((piece, width), bf16),
            jax.ShapeDtypeStruct((rows, columns), f32),
            jax.ShapeDtypeStruct((rows, columns), f32),
            jax.ShapeDtypeStruct(sum_taps.shape, f32),
        ),
        in_specs=[hbm] * 4 + [vmem] + [hbm] * 3 + [vmem],
        out_specs=(hbm, vmem, hbm, hbm, vmem),
        scratch_shapes=[
            pltpu.VMEM((strips, n * rows, 2 * LANE), bf16),
            pltpu.VMEM((tokens, width), bf16),
            pltpu.VMEM((tokens, width), bf16),
            pltpu.VMEM((width, tokens), bf16),
            pltpu.VMEM((strips, tokens, 2 * LANE), bf16),
            pltpu.VMEM((strips, tokens, LANE), bf16),
            pltpu.VMEM((2, tokens, LANE), bf16),
            pltpu.VMEM((2, depth, rows, 2 * LANE), bf16),
            pltpu.VMEM((strips, depth, rows, 2 * LANE), bf16),
            pltpu.VMEM((strips, hops, rows, 2 * LANE), bf16),
            pltpu.VMEM((strips, hops, rows, 2 * LANE), bf16),
            pltpu.VMEM((strips, rows, 2 * LANE), bf16),
            pltpu.VMEM((tokens, width), bf16),
            pltpu.VMEM((tp_n, piece, width), bf16),
            pltpu.VMEM(taps_shape, f32),
            pltpu.VMEM((n,) + taps_shape, f32),
            pltpu.VMEM(conv_taps.shape, f32),
            pltpu.VMEM((tokens, width), f32),
            pltpu.VMEM((rows, columns), f32),
            pltpu.VMEM((rows, columns), f32),
        ]
        + [sems((strips,))] * 2
        + [sems((strips, hops))] * 4
        + [sems((strips, depth))] * 2
        + [sems((strips,))] * 2
        + [sems((2,)), sems((strips,))]
        + [sems((2,)), sems((strips,))]
        + [sems((strips, depth)), sems((strips, hops)), sems((strips, hops))]
        + [sems((strips,))] * 2
        + [sems((tp_n, parts))] * 6
        + [sems((tp_n,))] * 2
        + [sems((n,))] * 2
        + [sems, sems]
        + [sems((2,)), sems((strips, 2))],
        compiler_params=pltpu.CompilerParams(
            collective_id=0, has_side_effects=True, vmem_limit_bytes=67043328
        ),
        name="layer",
    )(
        x_late, x_early, w_gate, w_value, conv_taps, grad_hidden, sum_gate, sum_value, sum_taps
    )


def solution(mesh):
    placed = (
        P(("fs", "tp"), None),
        P(("fs", "tp"), None),
        P("fs", "tp"),
        P("fs", "tp"),
        P(None, "tp"),
        P("fs", "tp"),
        P("fs", "tp"),
        P("fs", "tp"),
        P(None, "tp"),
    )
    return jax.shard_map(
        shards,
        mesh=mesh,
        in_specs=placed,
        out_specs=(
            P("fs", "tp"),
            P(("fs", "tp"), None),
            P("fs", "tp"),
            P("fs", "tp"),
            P(None, "tp"),
        ),
        check_vma=False,
    )
```

```python
import functools
import math

import jax
import jax.numpy as jnp
from jax import lax
from jax.experimental import pallas as pl
from jax.experimental.pallas import tpu as pltpu
from jax.sharding import PartitionSpec as P

root_half = 0.7071067811865476
density_norm = 0.3989422804014327
MESH = pl.DeviceIdType.MESH
LANE = 128
HOP = 2
BEHIND = 5
DELAY = 1
FLUSH = 1
LATER = 1
JOIN = (2, 4)
MEET = 3
GROUPS = (7, 3)
TURN = 2


def kernel(n, tp_n, factor, *refs):
    x_late, x_early, w_gate, w_value, conv, grad_hidden, sum_gate, sum_value, sum_taps = refs[:9]
    hidden, grad_early, new_gate, new_value, new_taps = refs[9:14]
    (
        strip, late_rows, early_rows, flipped, cots, upstream, out_stage, wire, part_got,
        up_got, down_got, fin_got, partial_got, taps_own, taps_got, conv_got, ahead,
        gate_total, value_total, mid_got, far_got,
    ) = refs[14:35]
    (
        w_out, w_in, up_out, up_in, down_out, down_in, share_out, share_in, u_out, u_in,
        h_out, h_in, q_out, q_in, z_out, zup_in, zdown_in, f_out, f_in, late_out, late_in,
        early_out, early_in, late_pass, early_pass, p_out, p_in, t_out, t_in, c_out, c_in,
        sums_in, sums_out, m_out, m_in, a_out, a_in,
    ) = refs[35:]
    partial = late_rows
    depth, half = n // 2, tp_n // 2
    rows, columns = gate_total.shape
    strips = columns // LANE
    tokens, width = early_rows.shape
    piece = x_early.shape[0]
    taps_count = conv.shape[0]
    lag = HOP + depth - 1
    late_at = lag + min(BEHIND, strips - 1 - (strips - 1) // 2)
    last_hop = lag + depth - 2
    flush = max(strips + lag - FLUSH, last_hop)
    ended = strips + lag - 1
    parts = early_in.shape[1]
    part = piece // parts
    groups = [0] + [strips - k for k in GROUPS if strips > k] + [strips]
    me, tp = lax.axis_index("fs"), lax.axis_index("tp")
    z, y = lax.div(me, 2), lax.rem(me, 2)
    x, c = lax.div(tp, 2), lax.rem(tp, 2)
    same = c == y
    other = jnp.logical_not(same)
    role_fs, role_tp = z * 2 + c, x * 2 + y
    twin = {"fs": role_fs, "tp": role_tp}
    partner = {"fs": me, "tp": x * 2 + 1 - c}
    above, below = {"fs": me + 2, "tp": tp}, {"fs": me - 2, "tp": tp}
    has_up, has_down = z + 1 < depth, z > 0

    def send(src, dst, out_sem, in_sem, to):
        return pltpu.make_async_remote_copy(
            src_ref=src, dst_ref=dst, send_sem=out_sem, recv_sem=in_sem,
            device_id=to, device_id_type=MESH,
        )

    def landed(dst, sem):
        pltpu.make_async_copy(dst, dst, sem).wait()

    def lanes(s):
        return pl.ds(pl.multiple_of(s * LANE, LANE), LANE)

    def block(zz, cc):
        return pl.ds(pl.multiple_of((zz * 2 + cc) * rows, rows), rows)

    def own_slot(s, zz, cc):
        return strip.at[s, block(zz, cc)]

    barrier = pltpu.get_barrier_semaphore()

    def hail(i, _):
        j = lax.rem(me * 2 + c + i, 2 * n)
        pl.semaphore_signal(
            barrier, inc=1, device_id={"fs": lax.div(j, 2), "tp": x * 2 + lax.rem(j, 2)},
            device_id_type=MESH,
        )
        return 0

    lax.fori_loop(1, 2 * n, hail, 0)
    for dx in range(1, half):
        for yy in range(2):
            for cc in range(2):
                pl.semaphore_signal(
                    barrier, inc=1,
                    device_id={"fs": z * 2 + yy, "tp": lax.rem(x + dx, half) * 2 + cc},
                    device_id_type=MESH,
                )
    pl.semaphore_wait(barrier, 2 * n - 1 + 4 * (half - 1))

    def weights_away(s, there):
        for source, at in ((w_gate, 0), (w_value, LANE)):
            src = source.at[:, lanes(s)]
            dst = strip.at[s, block(z, y), pl.ds(at, LANE)]
            if there:
                send(src, dst, w_out.at[s], w_in.at[s], twin).start()
            else:
                pltpu.make_async_copy(src, dst, w_in.at[s]).start()

    def weights_first(first, last):
        def body(s, _):
            pl.when(same)(lambda: weights_away(s, False))
            pl.when(other)(lambda: weights_away(s, True))
            return 0

        lax.fori_loop(first, last, body, 0)

    def upstream_copy(s):
        return send(grad_hidden.at[:, lanes(s)], upstream.at[s], u_out.at[s], u_in.at[s], twin)

    def upstream_first(s, _):
        @pl.when(same)
        def _():
            pltpu.make_async_copy(grad_hidden.at[:, lanes(s)], upstream.at[s], u_in.at[s]).start()

        pl.when(other)(lambda: upstream_copy(s).start())
        return 0

    def token_part(into, t, q):
        return into.at[pl.ds(pl.multiple_of(t * piece + q * part, part), part)]

    def token_copies(source, into, out_sem, in_sem, q):
        copies = []
        for i, (dx, yy) in enumerate([(0, 1 - y)] + [(dx, y) for dx in range(1, half)] + [(0, y)]):
            to = {"fs": z * 2 + yy, "tp": lax.rem(x + dx, half) * 2 + y}
            mine = same if i == half else None
            src = source.at[pl.ds(q * part, part)]
            copies.append((mine, src, token_part(into, tp, q), out_sem.at[i, q], in_sem.at[tp, q], to))
        return copies

    def tokens_start(copies):
        for mine, src, dst, out_sem, in_sem, to in copies:
            if mine is None:
                send(src, dst, out_sem, in_sem, to).start()
            else:
                pl.when(mine)(lambda: pltpu.make_async_copy(src, dst, in_sem).start())
                pl.when(jnp.logical_not(mine))(lambda: send(src, dst, out_sem, in_sem, to).start())

    def tokens_sent(copies):
        for mine, src, dst, out_sem, in_sem, to in copies:
            if mine is None:
                send(src, dst, out_sem, in_sem, to).wait_send()
            else:
                pl.when(jnp.logical_not(mine))(lambda: send(src, dst, out_sem, in_sem, to).wait_send())

    def turn(into, in_sem, pass_sem, cc, dx, q):
        t = x * 2 + cc
        at = token_part(into, t, q)
        to = {"fs": me, "tp": lax.rem(x + dx, half) * 2 + c}
        return send(at, at, pass_sem.at[cc * half + dx, q], in_sem.at[t, q], to)

    def tokens_turn(into, in_sem, pass_sem, q):
        @pl.when(other)
        def _():
            for cc in range(2):
                landed(token_part(into, x * 2 + cc, q), in_sem.at[x * 2 + cc, q])
                for dx in range(1, half):
                    turn(into, in_sem, pass_sem, cc, dx, q).start()

    def turned(into, in_sem, pass_sem):
        @pl.when(other)
        def _():
            for q in range(parts):
                for dx in range(1, half):
                    for cc in range(2):
                        turn(into, in_sem, pass_sem, cc, dx, q).wait_send()

    def tokens_here(into, in_sem):
        for t in range(tp_n):

            @pl.when(jnp.logical_or(same, x != t // 2))
            def _():
                for q in range(parts):
                    landed(token_part(into, t, q), in_sem.at[t, q])

    early_copies = [token_copies(x_early, early_rows, early_out, early_in, q) for q in range(parts)]
    late_copies = [token_copies(x_late, late_rows, late_out, late_in, q) for q in range(parts)]
    first = min(2, strips)
    weights_first(0, first)
    conv_copy = send(conv, conv_got, c_out, c_in, partner)
    conv_copy.start()
    for q in range(parts):
        tokens_start(early_copies[q])
        weights_first(min(first + q, strips), min(first + q + 1, strips))
    soon = min(first + parts, strips)
    head = min(4, strips)

    def second_wave():
        def body(s, _):
            pl.when(s < head)(lambda: (upstream_first(s, 0), None)[1])
            at = soon + 2 * s
            for i in range(2):
                pl.when(at + i < strips)(lambda: weights_first(at + i, at + i + 1))
            return 0

        lax.fori_loop(0, max(head, -(-(strips - soon) // 2)), body, 0)

    def third_wave():
        for q in range(parts):
            tokens_start(late_copies[q])
            lax.fori_loop(min(head + q, strips), min(head + q + 1, strips), upstream_first, 0)
        lax.fori_loop(min(head + parts, strips), strips, upstream_first, 0)

    def up(s, k):
        at = own_slot(s, z - k, c)
        return send(at, at, up_out.at[s, k], up_in.at[s, k], above)

    def down(s, k):
        at = own_slot(s, z + k, c)
        return send(at, at, down_out.at[s, k], down_in.at[s, k], below)

    def share(s, zz):
        at = own_slot(s, zz, c)
        return send(at, at, share_out.at[s, zz], share_in.at[s, zz], partner)

    def spread(s):
        landed(own_slot(s, z, c), w_in.at[s])
        pl.when(has_up)(lambda: up(s, 0).start())
        pl.when(has_down)(lambda: down(s, 0).start())
        share(s, z).start()

    def hop(s, k):
        @pl.when(z - 1 - k >= 0)
        def _():
            landed(own_slot(s, z - 1 - k, c), up_in.at[s, k])
            pl.when(has_up)(lambda: up(s, k + 1).start())
            share(s, z - 1 - k).start()

        @pl.when(z + 1 + k < depth)
        def _():
            landed(own_slot(s, z + 1 + k, c), down_in.at[s, k])
            pl.when(has_down)(lambda: down(s, k + 1).start())
            share(s, z + 1 + k).start()

    def gathered(s):
        def body(zz, _):
            landed(own_slot(s, zz, 1 - c), share_in.at[s, zz])
            return 0

        lax.fori_loop(0, depth, body, 0)

    def taps_of(s):
        got = jnp.where(same, conv[:, lanes(s)], conv_got[:, lanes(s)])
        return [got[j : j + 1] for j in range(taps_count)]

    def mix(gate, taps):
        position = lax.broadcasted_iota(jnp.int32, gate.shape, 0)
        moved = []
        for j in range(taps_count):
            delay = taps_count - 1 - j
            if delay == 0:
                moved.append(gate)
            else:
                moved.append(jnp.where(position >= delay, pltpu.roll(gate, delay, 0), 0.0))
        pre = moved[0] * taps[0]
        for j in range(1, taps_count):
            pre = pre + moved[j] * taps[j]
        return pre, moved

    def project(source, s):
        both = jnp.dot(source[...], strip[s], preferred_element_type=jnp.float32)
        both = both.astype(jnp.bfloat16).astype(jnp.float32)
        return both[:, :LANE], both[:, LANE:]

    def backward(s):
        landed(upstream.at[s], u_in.at[s])
        gate, value = project(early_rows, s)
        taps = taps_of(s)
        pre, moved = mix(gate, taps)
        cdf = 0.5 * (1.0 + lax.erf(pre * root_half))
        bend = cdf + pre * jnp.exp(-0.5 * pre * pre) * density_norm
        grad = upstream[s].astype(jnp.float32)
        cots[s, :, LANE:] = (grad * (pre * cdf)).astype(cots.dtype)
        slope = grad * value * bend
        for j in range(taps_count):
            taps_own[pl.ds(j, 1), lanes(s)] = jnp.sum(slope * moved[j], axis=0, keepdims=True)
        position = lax.broadcasted_iota(jnp.int32, slope.shape, 0)
        d_gate = slope * taps[taps_count - 1]
        for j in range(taps_count - 1):
            ahead = taps_count - 1 - j
            later = jnp.where(position < tokens - ahead, pltpu.roll(slope, tokens - ahead, 0), 0.0)
            d_gate = d_gate + later * taps[j]
        cots[s, :, :LANE] = d_gate.astype(cots.dtype)

    def terms(s, cc):
        made = factor * jnp.dot(flipped[cc], cots[s], preferred_element_type=jnp.float32)
        return made.reshape(depth, rows, 2 * LANE)

    def to_partner(s):
        slot = lax.rem(s, 2)
        return send(wire.at[slot], part_got.at[s], q_out.at[slot], q_in.at[s], partner)

    def terms_away(s):
        slot = lax.rem(s, 2)
        pl.when(s >= 2)(lambda: to_partner(s - 2).wait_send())

        wire[slot] = terms(s, 1 - c).astype(wire.dtype)
        to_partner(s).start()

    def terms_here(s):
        landed(part_got.at[s], q_in.at[s])
        part_got[s] = (terms(s, c) + part_got[s].astype(jnp.float32)).astype(part_got.dtype)

    def hidden_copy(s, there):
        slot = lax.rem(s, 2)
        src, dst = out_stage.at[slot], hidden.at[:, lanes(s)]
        if there:
            return send(src, dst, h_out.at[slot], h_in.at[s], twin)
        return pltpu.make_async_copy(src, dst, h_out.at[slot])

    def hidden_sent(s):
        pl.when(other)(lambda: hidden_copy(s, True).wait_send())
        pl.when(same)(lambda: hidden_copy(s, False).wait())

    def forward(s):
        slot = lax.rem(s, 2)
        pl.when(s >= 2)(lambda: hidden_sent(s - 2))
        gate, value = project(late_rows, s)
        pre, _ = mix(gate, taps_of(s))
        active = 0.5 * pre * (1.0 + lax.erf(pre * root_half))
        out_stage[slot] = (active * value).astype(out_stage.dtype)
        pl.when(other)(lambda: hidden_copy(s, True).start())
        pl.when(same)(lambda: hidden_copy(s, False).start())

    def along(s, zz, away, upward):
        got, sem, to = (up_got, zup_in, above) if upward else (down_got, zdown_in, below)
        return send(part_got.at[s, zz], got.at[s, away - 1], z_out.at[s, zz], sem.at[s, away - 1], to)

    def pass_on(s, away, upward):
        zz = z + away if upward else z - away
        inside = zz < depth if upward else zz >= 0
        got, sem = (up_got, zup_in) if upward else (down_got, zdown_in)

        @pl.when(inside)
        def _():
            if away < depth - 1:

                @pl.when(has_down if upward else has_up)
                def _():
                    landed(got.at[s, away], sem.at[s, away])
                    value = part_got[s, zz].astype(jnp.float32) + got[s, away].astype(jnp.float32)
                    part_got[s, zz] = value.astype(part_got.dtype)

            along(s, zz, away, upward).start()

    def fin(s):
        return send(part_got.at[s, z], fin_got.at[s], f_out.at[s], f_in.at[s], twin)

    sums = ((sum_gate, gate_total, new_gate), (sum_value, value_total, new_value))

    def sum_load(i):
        return pltpu.make_async_copy(sums[i][0], sums[i][1], sums_in.at[i])

    def sum_store(i, s):
        at = (slice(None), lanes(s))
        return pltpu.make_async_copy(sums[i][1].at[at], sums[i][2].at[at], sums_out.at[s, i])

    def put_total(s, value):
        gate_total[:, lanes(s)] += value[:, :LANE]
        value_total[:, lanes(s)] += value[:, LANE:]
        for i in range(2):
            sum_store(i, s).start()

    def finish(s):
        pl.when(has_down)(lambda: landed(up_got.at[s, 0], zup_in.at[s, 0]))
        pl.when(has_up)(lambda: landed(down_got.at[s, 0], zdown_in.at[s, 0]))

        def settle(value):
            pl.when(same)(lambda: put_total(s, value))

            @pl.when(other)
            def _():
                part_got[s, z] = value.astype(part_got.dtype)

        def total(refs_):
            value = part_got[s, z].astype(jnp.float32)
            for ref in refs_:
                value = value + ref[s, 0].astype(jnp.float32)
            settle(value)

        pl.when(jnp.logical_not(has_down))(lambda: total([down_got]))
        pl.when(jnp.logical_not(has_up))(lambda: total([up_got]))
        pl.when(jnp.logical_and(has_up, has_down))(lambda: total([up_got, down_got]))
        pl.when(other)(lambda: fin(s).start())

    def accept(s):
        @pl.when(other)
        def _():
            landed(fin_got.at[s], f_in.at[s])
            put_total(s, fin_got[s].astype(jnp.float32))

    wide = 2 * LANE
    blocks = width // wide

    def grad_block(b, first, last):
        at = pl.ds(pl.multiple_of(b * wide, wide), wide)
        total = jnp.zeros((tokens, wide), jnp.float32)
        for s in range(first, last):
            total = total + lax.dot_general(
                cots[s], strip[s, at, :], (((1,), (1,)), ((), ())), preferred_element_type=jnp.float32
            )
        return at, total

    def input_grad_ahead(s):
        for g in range(len(groups) - 2):
            start, end = groups[g + 1], groups[g + 2]
            share_of = -(-blocks // (end - start))

            @pl.when(jnp.logical_and(s >= start, s < end))
            def _():
                first = (s - start) * share_of

                def body(b, _):
                    at, total = grad_block(b, groups[g], start)
                    if g > 0:
                        total = total + ahead[:, at]
                    ahead[:, at] = total
                    return 0

                lax.fori_loop(jnp.minimum(first, blocks), jnp.minimum(first + share_of, blocks), body, 0)

    def input_grad():
        def body(b, _):
            at, total = grad_block(b, groups[-2], strips)
            if len(groups) > 2:
                total = total + ahead[:, at]
            partial[:, at] = total.astype(partial.dtype)
            return 0

        lax.fori_loop(0, blocks, body, 0)

    def partial_rows(t):
        return partial.at[pl.ds(pl.multiple_of(t * piece, piece), piece)]

    def partial_add(t, gots):
        at = pl.ds(pl.multiple_of(t * piece, piece), piece)
        total = partial[at, :].astype(jnp.float32)
        for got in gots:
            total = total + got[...].astype(jnp.float32)
        partial[at, :] = total.astype(partial.dtype)

    def direct(dx, cc):
        t = lax.rem(x + dx, half) * 2 + cc
        return send(
            partial_rows(t), partial_got.at[x], p_out.at[t], p_in.at[x], {"fs": me, "tp": t}
        )

    def direct_start(dx, cc):
        if dx > 0:
            direct(dx, cc).start()
        else:
            here = pltpu.make_async_copy(partial_rows(tp), partial_got.at[x], p_in.at[x])
            pl.when(cc == c)(lambda: here.start())
            pl.when(cc != c)(lambda: direct(dx, cc).start())

    def across(dx):
        xx = lax.rem(x + dx, half)
        return send(
            partial_rows(xx * 2), mid_got.at[dx - 1], m_out.at[dx - 1], m_in.at[dx - 1],
            {"fs": me, "tp": xx * 2 + c},
        )

    def over():
        return send(
            partial_rows(x * 2), partial_got.at[half], p_out.at[0], p_in.at[half],
            {"fs": role_fs, "tp": x * 2},
        )

    def away_y(dx):
        t = lax.rem(x + dx, half) * 2 + 1
        return send(
            partial_rows(t), far_got.at[dx], a_out.at[dx], a_in.at[dx], {"fs": role_fs, "tp": tp}
        )

    order = tuple(range(1, half)) + (0,)

    def partial_start():
        @pl.when(other)
        def _():
            for dx in range(1, half):
                across(dx).start()
            for dx in order:
                away_y(dx).start()

        pl.when(same)(lambda: direct_start(0, 0))

    def partial_far():
        @pl.when(same)
        def _():
            for dx in range(1, half):
                direct_start(dx, 0)

    def partial_joined(dx):
        @pl.when(same)
        def _():
            landed(far_got.at[dx], a_in.at[dx])
            partial_add(lax.rem(x + dx, half) * 2 + 1, [far_got.at[dx]])
            direct_start(dx, 1)

    def partial_over():
        @pl.when(other)
        def _():
            for dx in range(1, half):
                landed(mid_got.at[dx - 1], m_in.at[dx - 1])
            if half > 1:
                partial_add(x * 2, [mid_got.at[dx - 1] for dx in range(1, half)])
            over().start()

    def partial_sent():
        @pl.when(same)
        def _():
            for dx in range(half):
                for cc in range(2):
                    if dx > 0:
                        direct(dx, cc).wait_send()
                    else:
                        pl.when(cc != c)(lambda: direct(dx, cc).wait_send())

        @pl.when(other)
        def _():
            over().wait_send()
            for dx in range(half):
                away_y(dx).wait_send()
                if dx > 0:
                    across(dx).wait_send()

    def partial_total():
        for i in range(half):
            landed(partial_got.at[i], p_in.at[i])
        total = partial_got[0].astype(jnp.float32)
        for i in range(1, half):
            total = total + partial_got[i].astype(jnp.float32)

        @pl.when(c == 1)
        def _():
            partial_got[0] = total.astype(partial_got.dtype)

        @pl.when(c == 0)
        def _():
            landed(partial_got.at[half], p_in.at[half])
            whole = total + partial_got[half].astype(jnp.float32)
            partial_got[0] = whole.astype(partial_got.dtype)

        out = pltpu.make_async_copy(partial_got.at[0], grad_early, sums_in.at[0])
        out.start()
        out.wait()

    def taps_copies(fn_there, fn_here):
        def body(f, _):
            copy = send(
                taps_own, taps_got.at[role_fs], t_out.at[f], t_in.at[role_fs],
                {"fs": f, "tp": role_tp},
            )
            here = jnp.logical_and(same, f == me)
            pl.when(jnp.logical_not(here))(lambda: fn_there(copy))
            if fn_here is not None:
                pl.when(here)(
                    lambda: fn_here(pltpu.make_async_copy(taps_own, taps_got.at[role_fs], t_in.at[role_fs]))
                )
            return 0

        lax.fori_loop(0, n, body, 0)

    def gather_sent(s, _):
        @pl.when(other)
        def _():
            landed(own_slot(s, z, c), w_out.at[s])
            upstream_copy(s).wait_send()

        for k in range(depth - 1):
            pl.when(jnp.logical_and(has_up, z - k >= 0))(lambda k=k: up(s, k).wait_send())
            pl.when(jnp.logical_and(has_down, z + k < depth))(lambda k=k: down(s, k).wait_send())
        lax.fori_loop(0, depth, lambda zz, _: (share(s, zz).wait_send(), 0)[1], 0)
        return 0

    for i in range(2):
        sum_load(i).start()

    def guarded(s, work):
        pl.when(jnp.logical_and(s >= 0, s < strips))(lambda: (work(s), None)[1])

    def prepare():
        for i in range(2):
            sum_load(i).wait()
        tokens_here(early_rows, early_in)
        conv_copy.wait_recv()
        taps_own[...] = jnp.zeros(taps_own.shape, jnp.float32)
        part_rows = min(rows, wide)
        for b in range(width // wide):
            turned_block = early_rows[:, b * wide : (b + 1) * wide].T
            for first in range(0, wide, part_rows):
                f, at = divmod(b * wide + first, rows)
                flipped[f % 2, pl.ds(f // 2 * rows + at, part_rows), :] = turned_block[
                    first : first + part_rows
                ]

    def delayed(t, at, steps, work):
        until = flush + at - last_hop
        pl.when(t < until)(lambda: guarded(t - at - steps, work))

        @pl.when(t == until)
        def _():
            lax.fori_loop(
                jnp.maximum(0, until - at - steps), min(strips, until - at),
                lambda s, _: (work(s), 0)[1], 0,
            )

        pl.when(t >= until)(lambda: guarded(t - at, work))

    def strip_work(s):
        pl.when(s == 0)(prepare)
        gathered(s)
        backward(s)
        terms_away(s)

    def late_work(s):
        pl.when(s == 0)(lambda: tokens_here(late_rows, late_in))
        forward(s)

    def own_work(s):
        terms_here(s)
        for upward in (True, False):
            pass_on(s, depth - 1, upward)
        input_grad_ahead(s)

    def step(t, _):
        guarded(t, spread)
        for k in range(depth - 1):
            guarded(t - HOP - k, lambda s, k=k: hop(s, k))

        for q in range(parts):
            pl.when(t == min(1 + (q + 1) // 2, lag - 1))(
                lambda: tokens_turn(early_rows, early_in, early_pass, q)
            )
            pl.when(t == min(lag + TURN + q, late_at - 1))(
                lambda: tokens_turn(late_rows, late_in, late_pass, q)
            )
        pl.when(t == min(3, lag - 1))(second_wave)
        guarded(t - lag, strip_work)

        for j in range(2):
            guarded(2 * (t - late_at) + j, late_work)
        guarded(t - lag, own_work)
        pl.when(t == lag)(third_wave)

        @pl.when(t == ended)
        def _():
            conv_copy.wait_send()
            for q in range(parts):
                tokens_sent(early_copies[q])
                tokens_sent(late_copies[q])
            turned(early_rows, early_in, early_pass)
            turned(late_rows, late_in, late_pass)
            taps_copies(lambda copy: copy.start(), lambda copy: copy.start())
            input_grad()
            partial_start()

        for away in range(depth - 2, 0, -1):
            for upward in (True, False):
                links = z if upward else depth - 1 - z
                delayed(
                    t, lag + depth - 1 - away, DELAY * links, lambda s: pass_on(s, away, upward)
                )
        pl.when(t == ended + LATER)(partial_far)
        for dx in range(1, half):
            pl.when(t == ended + JOIN[0])(lambda: partial_joined(dx))
        pl.when(t == ended + MEET)(partial_over)
        pl.when(t == ended + JOIN[1])(lambda: partial_joined(0))
        links = jnp.maximum(jnp.where(has_down, z - 1, 0), jnp.where(has_up, depth - 2 - z, 0))
        delayed(t, last_hop + 1, DELAY * links, finish)
        delayed(t, last_hop + 2, DELAY * links, accept)

        @pl.when(t == ended)
        def _():
            lax.fori_loop(0, strips, gather_sent, 0)

        return 0

    steps = max(ended + 1 + depth, ended + 1 + max(*JOIN, MEET, LATER), late_at + strips // 2 + 1)
    lax.fori_loop(0, steps, step, 0)

    def taps_arrive(f, _):
        landed(taps_got.at[f], t_in.at[f])
        return 0

    lax.fori_loop(0, n, taps_arrive, 0)
    sum_of = taps_got[0]
    for i in range(1, n):
        sum_of = sum_of + taps_got[i]
    new_taps[...] = sum_taps[...] + factor * sum_of[:taps_count]

    taps_copies(lambda copy: copy.wait_send(), None)
    for s in range(max(0, strips - 2), strips):
        to_partner(s).wait_send()
        hidden_sent(s)

    def drain(s, _):
        for i in range(2):
            sum_store(i, s).wait()

        @pl.when(other)
        def _():
            hidden_copy(s, True).wait_recv()
            fin(s).wait_send()

        for away in range(1, depth):
            pl.when(z + away < depth)(lambda away=away: along(s, z + away, away, True).wait_send())
            pl.when(z - away >= 0)(lambda away=away: along(s, z - away, away, False).wait_send())
        return 0

    lax.fori_loop(0, strips, drain, 0)
    partial_total()
    partial_sent()


def out_kernel(halves, *refs):
    count = len(halves)
    sources, targets, held = refs[:count], refs[count : 2 * count], refs[2 * count : 3 * count]
    in_sem, out_sem = refs[3 * count :]
    copies = []
    for i, cuts in enumerate(halves):
        size = sources[i].shape[0] // cuts
        for k in range(cuts):
            at = pl.ds(k * size, size)
            j = len(copies)
            copies.append(
                (
                    pltpu.make_async_copy(sources[i].at[at], held[i].at[at], in_sem.at[j]),
                    pltpu.make_async_copy(held[i].at[at], targets[i].at[at], out_sem.at[j]),
                )
            )
    for there, _ in copies:
        there.start()
    for there, back in copies:
        there.wait()
        back.start()
    for _, back in copies:
        back.wait()


def hand_out(results):
    halves = tuple(2 if r.shape[0] % 32 == 0 else 1 for r in results)
    hbm = pl.BlockSpec(memory_space=pl.ANY)
    sems = pltpu.SemaphoreType.DMA((sum(halves),))
    return pl.pallas_call(
        functools.partial(out_kernel, halves),
        out_shape=tuple(jax.ShapeDtypeStruct(r.shape, r.dtype) for r in results),
        in_specs=[hbm] * len(results),
        out_specs=(hbm,) * len(results),
        scratch_shapes=[pltpu.VMEM(r.shape, r.dtype) for r in results] + [sems, sems],
        name="hand_out",
    )(*results)


def shards(x_late, x_early, w_gate, w_value, conv_taps, grad_hidden, sum_gate, sum_value, sum_taps):
    n, tp_n = lax.axis_size("fs"), lax.axis_size("tp")
    piece, width = x_early.shape
    rows, columns = w_gate.shape
    tokens = piece * tp_n
    strips, depth = columns // LANE, n // 2
    factor = 1.0 / math.sqrt(tokens * n)
    bf16, f32 = x_early.dtype, jnp.float32
    sems = pltpu.SemaphoreType.DMA
    vmem = pl.BlockSpec(memory_space=pltpu.VMEM)
    hbm = pl.BlockSpec(memory_space=pl.ANY)
    taps_shape = (8, columns)
    hops, half = depth - 1, tp_n // 2
    parts = next(q for q in (4, 2, 1) if piece % (16 * q) == 0)
    results = pl.pallas_call(
        functools.partial(kernel, n, tp_n, factor),
        out_shape=(
            jax.ShapeDtypeStruct((tokens, columns), bf16),
            jax.ShapeDtypeStruct((piece, width), bf16),
            jax.ShapeDtypeStruct((rows, columns), f32),
            jax.ShapeDtypeStruct((rows, columns), f32),
            jax.ShapeDtypeStruct(sum_taps.shape, f32),
        ),
        in_specs=[hbm] * 4 + [vmem] + [hbm] * 3 + [vmem],
        out_specs=(hbm,) * 4 + (vmem,),
        scratch_shapes=[
            pltpu.VMEM((strips, n * rows, 2 * LANE), bf16),
            pltpu.VMEM((tokens, width), bf16),
            pltpu.VMEM((tokens, width), bf16),
            pltpu.VMEM((2, width // 2, tokens), bf16),
            pltpu.VMEM((strips, tokens, 2 * LANE), bf16),
            pltpu.VMEM((strips, tokens, LANE), bf16),
            pltpu.VMEM((2, tokens, LANE), bf16),
            pltpu.VMEM((2, depth, rows, 2 * LANE), bf16),
            pltpu.VMEM((strips, depth, rows, 2 * LANE), bf16),
            pltpu.VMEM((strips, hops, rows, 2 * LANE), bf16),
            pltpu.VMEM((strips, hops, rows, 2 * LANE), bf16),
            pltpu.VMEM((strips, rows, 2 * LANE), bf16),
            pltpu.VMEM((half + 1, piece, width), bf16),
            pltpu.VMEM(taps_shape, f32),
            pltpu.VMEM((n,) + taps_shape, f32),
            pltpu.VMEM(conv_taps.shape, f32),
            pltpu.VMEM((tokens, width), f32),
            pltpu.VMEM((rows, columns), f32),
            pltpu.VMEM((rows, columns), f32),
            pltpu.VMEM((max(half - 1, 1), piece, width), bf16),
            pltpu.VMEM((half, piece, width), bf16),
        ]
        + [sems((strips,))] * 2
        + [sems((strips, hops))] * 4
        + [sems((strips, depth))] * 2
        + [sems((strips,))] * 2
        + [sems((2,)), sems((strips,))]
        + [sems((2,)), sems((strips,))]
        + [sems((strips, depth)), sems((strips, hops)), sems((strips, hops))]
        + [sems((strips,))] * 2
        + [sems((tp_n, parts))] * 6
        + [sems((tp_n,))] * 2
        + [sems((n,))] * 2
        + [sems, sems]
        + [sems((2,)), sems((strips, 2))]
        + [sems((max(half - 1, 1),))] * 2
        + [sems((half,))] * 2,
        compiler_params=pltpu.CompilerParams(
            collective_id=0, has_side_effects=True, vmem_limit_bytes=67043328
        ),
        name="layer",
    )(
        x_late, x_early, w_gate, w_value, conv_taps, grad_hidden, sum_gate, sum_value, sum_taps
    )
    return hand_out(results)


def solution(mesh):
    placed = (
        P(("fs", "tp"), None),
        P(("fs", "tp"), None),
        P("fs", "tp"),
        P("fs", "tp"),
        P(None, "tp"),
        P("fs", "tp"),
        P("fs", "tp"),
        P("fs", "tp"),
        P(None, "tp"),
    )
    return jax.shard_map(
        shards,
        mesh=mesh,
        in_specs=placed,
        out_specs=(
            P("fs", "tp"),
            P(("fs", "tp"), None),
            P("fs", "tp"),
            P("fs", "tp"),
            P(None, "tp"),
        ),
        check_vma=False,
    )
```
